256 devices in a mesh: grp: 2 (over y), sp: 32 (over z, core), tp: 4 (over x).
Axes of the slice: x: 4, y: 2, z: 16, core: 2. Of those that a mesh axis runs over, the one named last changes fastest.
The devices are a block of a 4x16x16 slice.
Arguments:
- resid_in: bfloat16 [16384, 2048], P(('grp', 'sp', 'tp')), parts along dimension 0, may hold values from -6 to 6
- query_narrow: bfloat16 [16384, 8, 128], P(('grp', 'sp'), 'tp'), parts along dimension 0, may hold values from -512 to 512
- key_narrow: bfloat16 [16384, 4, 128], P(('grp', 'sp'), 'tp'), parts along dimension 0, may hold values from -512 to 512
- value_narrow: bfloat16 [16384, 4, 128], P(('grp', 'sp'), 'tp'), parts along dimension 0, may hold values from -6 to 6
- query_wide: bfloat16 [16384, 8, 256], P(('grp', 'sp'), 'tp'), parts along dimension 0, may hold values from -512 to 512
- key_wide: bfloat16 [16384, 4, 256], P(('grp', 'sp'), 'tp'), parts along dimension 0, may hold values from -512 to 512
- value_wide: bfloat16 [16384, 4, 128], P(('grp', 'sp'), 'tp'), parts along dimension 0, may hold values from -6 to 6
- lambda_narrow: float32 [8], P('tp'), may hold values from 0.3 to 0.8
- lambda_wide: float32 [8], P('tp'), may hold values from 0.3 to 0.8
- head_gain: float32 [128], replicated, may hold values from 0.1 to 1.9
- out_narrow: bfloat16 [1024, 2048], P('tp'), may hold values from -0.125 to 0.125
- out_wide: bfloat16 [1024, 2048], P('tp'), may hold values from -0.125 to 0.125
- norm_gain: bfloat16 [2048], replicated, may hold values from 0.099609375 to 1.8984375
- up_weight: bfloat16 [2048, 8192], P('sp', 'tp'), may hold values from -0.125 to 0.125
- down_weight: bfloat16 [8192, 2048], P('tp', 'sp'), may hold values from -0.0625 to 0.0625
Outputs:
- mixed_out: bfloat16 [16384, 2048], P(('grp', 'sp', 'tp')), parts along dimension 0
The draws below stay inside these ranges and needn't reach their ends.
There are 2 independent parts, one for each index of `grp`. The reference program is written for one: setup_inputs(seed, part) draws one part's arguments, and reference() takes and returns one part's arrays. A program takes and returns all parts, laid end to end along the dimension named above; an argument that names none is the same for every part. Nothing has to cross between parts.
All inputs are finite; a program needn't handle non-finite values.
Results may differ from the reference program's by a relative error of at most 0.018.
Values may be sent and summed in bfloat16 or wider, within the bound.
No kernel may reach another device: no remote copies, remote signals or barrier semaphores. Data moves between devices by JAX's collectives and lax.ppermute only.
A program may use at most 128 MiB of HBM per device.

```python
import math
import jax
import jax.numpy as jnp
from jax import lax

D = 2048
FF = 8192
HN = 8
DN = 64
KN = 4
HW = 8
DW = 128
KW = 4
DV = 128
SEQ = 8192
N_TP = 4


SPREAD = 1.32


def paired_draw(base_key, head_count, key_head_stack, half_width):
    full_width = 2 * half_width
    query_draw, keys_draw = jax.random.split(base_key, 2)
    key_rows = jnp.clip(jax.random.normal(keys_draw, (SEQ, key_head_stack, full_width), jnp.float32) * SPREAD, -4.0 * SPREAD, 4.0 * SPREAD)
    query_rows_all = jnp.clip(jax.random.normal(query_draw, (SEQ, head_count, full_width), jnp.float32) * SPREAD, -4.0 * SPREAD, 4.0 * SPREAD)
    return (query_rows_all, key_rows)


def draw_query_narrow(key, part):
    return paired_draw(jax.random.fold_in(key, 101), HN, KN, DN)[0].astype(jnp.bfloat16)


def draw_key_narrow(key, part):
    return paired_draw(jax.random.fold_in(key, 101), HN, KN, DN)[1].astype(jnp.bfloat16)


def draw_query_wide(key, part):
    return paired_draw(jax.random.fold_in(key, 202), HW, KW, DW)[0].astype(jnp.bfloat16)


def draw_key_wide(key, part):
    return paired_draw(jax.random.fold_in(key, 202), HW, KW, DW)[1].astype(jnp.bfloat16)


def steps_of(rng, shape, cuts, smallest, high):
    level = 1.0
    for dim, shards_of in cuts:
        steps = jax.random.uniform(jax.random.fold_in(jax.random.fold_in(rng, 6), dim), (shards_of,), jnp.float32, smallest / len(cuts), high / len(cuts))
        level = level * jnp.repeat(jnp.exp(steps), shape[dim] // shards_of).reshape((-1,) + (1,) * (len(shape) - 1 - dim))
    return level


def scatter_about(key, dims, spread, limit, cuts=(), held_as=jnp.bfloat16):
    result = jax.random.normal(key, dims, jnp.float32) * spread
    if len(cuts) > 0:
        result = steps_of(key, dims, cuts, -0.22, 0.18) * result
    return jnp.clip(result, min=-limit, max=limit).astype(held_as)


def setup_inputs(seed: int = 0, part: int = 0) -> dict:
    streams_of = jax.random.split(jax.random.key(seed), 16)
    part_splits = jax.random.split(jax.random.fold_in(streams_of[15], part), 16)
    return {
        "resid_in": scatter_about(part_splits[0], (SEQ, D), 1.0, 6.0, ((0, 128),)),
        "query_narrow": draw_query_narrow(jax.random.fold_in(jax.random.fold_in(streams_of[15], part), 71), part),
        "key_narrow": draw_key_narrow(jax.random.fold_in(jax.random.fold_in(streams_of[15], part), 71), part),
        "value_narrow": scatter_about(part_splits[3], (SEQ, KN, DV), 1.0, 6.0, ((0, 32), (1, 4))),
        "query_wide": draw_query_wide(jax.random.fold_in(jax.random.fold_in(streams_of[15], part), 71), part),
        "key_wide": draw_key_wide(jax.random.fold_in(jax.random.fold_in(streams_of[15], part), 71), part),
        "value_wide": scatter_about(part_splits[6], (SEQ, KW, DV), 1.0, 6.0, ((0, 32), (1, 4))),
        "lambda_narrow": jnp.clip(0.3 + 0.5 * jax.random.uniform(streams_of[7], (HN,), jnp.float32) ** steps_of(streams_of[7], (HN,), ((0, 4),), -0.2, 0.2), 0.3, 0.8),
        "lambda_wide": jnp.clip(0.3 + 0.5 * jax.random.uniform(streams_of[8], (HW,), jnp.float32) ** steps_of(streams_of[8], (HW,), ((0, 4),), -0.2, 0.2), 0.3, 0.8),
        "head_gain": jnp.clip(1.0 + 0.18 * jax.random.normal(streams_of[9], (DV,), jnp.float32), 0.1, 1.9),
        "out_narrow": scatter_about(streams_of[10], (HN * DV, D), ((HN + HW) * DV) ** -0.5, 0.125, ((0, 4),)),
        "out_wide": scatter_about(streams_of[11], (HW * DV, D), ((HN + HW) * DV) ** -0.5, 0.125, ((0, 4),)),
        "norm_gain": jnp.clip(1.0 + 0.18 * jax.random.normal(streams_of[12], (D,), jnp.float32), 0.099609375, 1.8984375).astype(jnp.bfloat16),
        "up_weight": scatter_about(streams_of[13], (D, FF), D ** -0.5, 0.125, ((0, 32), (1, 4))),
        "down_weight": scatter_about(streams_of[14], (FF, D), FF ** -0.5, 0.0625, ((0, 4), (1, 32))),
    }


NORM_EPS = 1e-06
OUT_SCALE = 0.8

def attend_ref(query, key_rows, values, lambdas, gain_vec):
    seq_len, head_count, full_width = query.shape
    key_head_stack = key_rows.shape[1]
    half_width = full_width // 2
    group_size = head_count // key_head_stack
    value_width = values.shape[2]
    block_rows = math.gcd(seq_len, 128)
    rotation_count = seq_len // block_rows
    key_float32 = key_rows.astype(jnp.float32).reshape(seq_len, key_head_stack, 2, half_width)
    value_float32 = values.astype(jnp.float32)
    query_blocks = query.reshape(rotation_count, block_rows, key_head_stack, group_size, 2, half_width)
    lambda_grid = lambdas.reshape(key_head_stack, group_size)[:, :, None, None]

    def per_block(query_blk):
        scores = jnp.einsum('tkgcd,skcd->kgcts', query_blk.astype(jnp.float32), key_float32) * half_width ** (-0.5)
        row_top = lax.optimization_barrier(jnp.max(scores, axis=-1, keepdims=True))
        powers = jnp.exp(scores - row_top)
        row_total = lax.optimization_barrier(jnp.sum(powers, axis=-1))
        rounded_result = lax.optimization_barrier(powers.astype(jnp.bfloat16)).astype(jnp.float32)
        weighted_values = jnp.einsum('iodph,hie->iodpe', rounded_result, value_float32)
        first_map = weighted_values[:, :, 0] / row_total[:, :, 0, :, None]
        second_map = weighted_values[:, :, 1] / row_total[:, :, 1, :, None]
        mixed = first_map - lambda_grid * second_map
        normed = mixed * lax.rsqrt(lax.optimization_barrier(jnp.mean(mixed * mixed, axis=-1, keepdims=True)) + NORM_EPS) * gain_vec * OUT_SCALE
        normed = normed.astype(jnp.bfloat16).transpose(2, 0, 1, 3)
        return normed.reshape(block_rows, head_count, value_width)
    outcome = lax.map(per_block, query_blocks)
    return outcome.reshape(seq_len, head_count * value_width)

def rounded_add(running, partial_value):
    return running + lax.optimization_barrier(partial_value.astype(jnp.bfloat16)).astype(jnp.float32)

def reference(resid_in, query_narrow, key_narrow, value_narrow, query_wide, key_wide, value_wide, lambda_narrow, lambda_wide, head_gain, out_narrow, out_wide, norm_gain, up_weight, down_weight):
    att_narrow = attend_ref(query_narrow, key_narrow, value_narrow, lambda_narrow, head_gain)
    att_wide = attend_ref(query_wide, key_wide, value_wide, lambda_wide, head_gain)
    narrow_cols = att_narrow.shape[1] // N_TP
    wide_cols = att_wide.shape[1] // N_TP
    projected = jnp.zeros(resid_in.shape, jnp.float32)
    for part_index in range(N_TP):
        low_n = part_index * narrow_cols
        low_w = part_index * wide_cols
        partial_value = jnp.dot(att_narrow[:, low_n:low_n + narrow_cols], out_narrow[low_n:low_n + narrow_cols], preferred_element_type=jnp.float32)
        partial_value = partial_value + jnp.dot(att_wide[:, low_w:low_w + wide_cols], out_wide[low_w:low_w + wide_cols], preferred_element_type=jnp.float32)
        projected = rounded_add(projected, partial_value)
    middle = (resid_in.astype(jnp.float32) + projected).astype(jnp.bfloat16)
    middle_f32 = middle.astype(jnp.float32)
    normed = middle_f32 * lax.rsqrt(lax.optimization_barrier(jnp.mean(middle_f32 * middle_f32, axis=-1, keepdims=True)) + NORM_EPS)
    normed = (normed * norm_gain.astype(jnp.float32)).astype(jnp.bfloat16)
    hidden_cols = up_weight.shape[1] // N_TP
    mixer = jnp.zeros(resid_in.shape, jnp.float32)
    for part_index in range(N_TP):
        low_h = part_index * hidden_cols
        lifted = jnp.dot(normed, up_weight[:, low_h:low_h + hidden_cols], preferred_element_type=jnp.float32)
        activated = jnp.square(jax.nn.relu(lifted)).astype(jnp.bfloat16)
        partial_value = jnp.dot(activated, down_weight[low_h:low_h + hidden_cols], preferred_element_type=jnp.float32)
        mixer = rounded_add(mixer, partial_value)
    return (middle_f32 + mixer).astype(jnp.bfloat16)
```

```python
import functools
import math

import jax
import jax.numpy as jnp
from jax import lax
from jax.experimental import pallas as pl
from jax.experimental.pallas import tpu as pltpu
from jax.sharding import PartitionSpec as P

NORM_EPS = 1e-06
OUT_SCALE = 0.8
LOG2E = math.log2(math.e)
LAST_DIMS = (((1,), (1,)), ((), ()))
VMEM_LIMIT = 60 * 2**20


def split_up(array, dim, peers):
    before, after = (array.shape[:dim], array.shape[dim + 1 :])
    return jnp.moveaxis(array.reshape(*before, peers, -1, *after), dim, 0)


def sent_and_summed(array, axis, dim):
    peers = lax.axis_size(axis)
    parts = lax.all_to_all(split_up(array, dim, peers), axis, 0, 0, tiled=True)
    return jnp.sum(parts.astype(jnp.float32), axis=0)


def copy_for_each(array, axis):
    copies = jnp.broadcast_to(array, (lax.axis_size(axis), *array.shape))
    return lax.all_to_all(copies, axis, split_axis=0, concat_axis=0, tiled=True)


def attend_kernel(
    qn_ref, qw_ref, kv_ref, lam_ref, gain_ref, out_ref, q_s, m_s, acc_s, v_s, *, dn, dw, dv, steps
):
    step = pl.program_id(0)
    rows = qn_ref.shape[0]

    @pl.when(step == 0)
    def _():
        m_s[...] = jnp.full_like(m_s, -jnp.inf)
        acc_s[...] = jnp.zeros_like(acc_s)
        v_s[...] = jnp.ones_like(v_s)
        lane = lax.broadcasted_iota(jnp.int32, (rows, 2 * dn), 1)
        for h in range(2):
            q = qn_ref[:, h * 2 * dn : (h + 1) * 2 * dn]
            for c in range(2):
                keep = (lane < dn) if c == 0 else (lane >= dn)
                q_s[h * 2 + c] = jnp.where(keep, q, jnp.zeros_like(q))
                q_s[4 + h * 2 + c] = qw_ref[:, (h * 2 + c) * dw : (h * 2 + c + 1) * dw]

    at_vn = 2 * dn
    at_kw = at_vn + dv
    at_vw = at_kw + 2 * dw
    v_s[0, :, :dv] = kv_ref[:, at_vn : at_vn + dv]
    v_s[1, :, :dv] = kv_ref[:, at_vw : at_vw + dv]
    for u in range(8):
        wide, c = u >= 4, u % 2
        at = at_kw + c * dw if wide else 0
        width = dw if wide else 2 * dn
        scale = (dw if wide else dn) ** -0.5 * LOG2E
        s = lax.dot_general(
            q_s[u], kv_ref[:, at : at + width], LAST_DIMS, preferred_element_type=jnp.float32
        )
        m_old = m_s[u]
        m_new = jnp.maximum(m_old, jnp.max(s, axis=1, keepdims=True))
        powers = jnp.exp2((s - m_new) * scale).astype(jnp.bfloat16)
        rescale = jnp.exp2((m_old - m_new) * scale)
        m_s[u] = m_new
        acc_s[u] = acc_s[u] * rescale + jnp.dot(
            powers, v_s[int(wide)], preferred_element_type=jnp.float32
        )

    @pl.when(step == steps - 1)
    def _():
        for h in range(4):
            first, second = acc_s[2 * h], acc_s[2 * h + 1]
            o = first[:, :dv] / first[:, dv:] - lam_ref[h] * (second[:, :dv] / second[:, dv:])
            square = jnp.mean(o * o, axis=-1, keepdims=True)
            o = o * lax.rsqrt(square + NORM_EPS) * gain_ref[...] * OUT_SCALE
            out_ref[:, h * dv : (h + 1) * dv] = o.astype(out_ref.dtype)


def attention(qn, qw, kv, lam, gain):
    rows = qn.shape[0]
    keys, width = kv.shape
    dv = gain.shape[1]
    dn, dw = qn.shape[1] // 4, qw.shape[1] // 4
    block = math.gcd(keys, 2048)
    steps = keys // block
    return pl.pallas_call(
        functools.partial(attend_kernel, dn=dn, dw=dw, dv=dv, steps=steps),
        grid=(steps,),
        in_specs=[
            pl.BlockSpec(qn.shape, lambda i: (0, 0)),
            pl.BlockSpec(qw.shape, lambda i: (0, 0)),
            pl.BlockSpec((block, width), lambda i: (i, 0)),
            pl.BlockSpec(memory_space=pltpu.SMEM),
            pl.BlockSpec(gain.shape, lambda i: (0, 0)),
        ],
        out_specs=pl.BlockSpec((rows, 4 * dv), lambda i: (0, 0)),
        out_shape=jax.ShapeDtypeStruct((rows, 4 * dv), jnp.bfloat16),
        scratch_shapes=[
            pltpu.VMEM((8, rows, 128), jnp.bfloat16),
            pltpu.VMEM((8, rows, 1), jnp.float32),
            pltpu.VMEM((8, rows, 2 * dv), jnp.float32),
            pltpu.VMEM((2, block, 2 * dv), jnp.bfloat16),
        ],
        compiler_params=pltpu.CompilerParams(
            dimension_semantics=("arbitrary",), vmem_limit_bytes=VMEM_LIMIT
        ),
        cost_estimate=pl.CostEstimate(
            flops=16 * rows * keys * 256, bytes_accessed=keys * width * 2, transcendentals=8 * rows * keys
        ),
        name="attend",
    )(qn, qw, kv, lam, gain)


def mixer_kernel(x_ref, w_ref, out_ref, lifted, activated, *, half):
    step = pl.program_id(0)
    depth = w_ref.shape[0] * w_ref.shape[2]
    w = w_ref[...].reshape(depth, w_ref.shape[3])

    @pl.when(step < half)
    def _():
        at = pl.multiple_of(step * depth, depth)
        part = jnp.dot(x_ref[:, pl.ds(at, depth)], w, preferred_element_type=jnp.float32)

        @pl.when(step == 0)
        def _():
            lifted[...] = part

        @pl.when(step > 0)
        def _():
            lifted[...] += part

    @pl.when(step == half - 1)
    def _():
        up = jnp.maximum(lifted[...], 0.0)
        activated[...] = (up * up).astype(jnp.bfloat16)

    @pl.when(step >= half)
    def _():
        out_ref[...] = lax.dot_general(
            activated[...], w, LAST_DIMS, preferred_element_type=jnp.float32
        ).astype(jnp.bfloat16)


def mixer(x, w):
    rows, d = x.shape
    shards, _, each, hidden = w.shape
    group = math.gcd(shards, 8)
    half = shards // group
    depth = group * each
    return pl.pallas_call(
        functools.partial(mixer_kernel, half=half),
        grid=(2 * half,),
        in_specs=[
            pl.BlockSpec((rows, d), lambda i: (0, 0)),
            pl.BlockSpec((group, 1, each, hidden), lambda i: (i % half, i // half, 0, 0)),
        ],
        out_specs=pl.BlockSpec((rows, depth), lambda i: (0, jnp.maximum(i - half, 0))),
        out_shape=jax.ShapeDtypeStruct((rows, d), jnp.bfloat16),
        scratch_shapes=[
            pltpu.VMEM((rows, hidden), jnp.float32),
            pltpu.VMEM((rows, hidden), jnp.bfloat16),
        ],
        compiler_params=pltpu.CompilerParams(
            dimension_semantics=("arbitrary",), vmem_limit_bytes=VMEM_LIMIT
        ),
        cost_estimate=pl.CostEstimate(
            flops=4 * rows * d * hidden, bytes_accessed=4 * d * hidden, transcendentals=0
        ),
        name="mixer",
    )(x, w)


def shards(
    resid_in,
    query_narrow,
    key_narrow,
    value_narrow,
    query_wide,
    key_wide,
    value_wide,
    lambda_narrow,
    lambda_wide,
    head_gain,
    out_narrow,
    out_wide,
    norm_gain,
    up_weight,
    down_weight,
):
    rows = query_narrow.shape[0]
    own = jnp.concatenate(
        [a.reshape(rows, -1) for a in (key_narrow, value_narrow, key_wide, value_wide)], axis=1
    )
    kv = lax.all_gather(own, "sp", axis=0, tiled=True)
    own_weights = jnp.stack([up_weight, down_weight.T])
    weights = lax.all_gather(own_weights, "sp", axis=0, tiled=False)
    attended = attention(
        query_narrow.reshape(rows, -1),
        query_wide.reshape(rows, -1),
        kv,
        jnp.concatenate([lambda_narrow, lambda_wide]),
        head_gain.reshape(1, -1),
    )
    out_rows = jnp.concatenate([out_narrow, out_wide], axis=0)
    projected = sent_and_summed(
        jnp.dot(attended, out_rows, preferred_element_type=jnp.float32).astype(jnp.bfloat16), "tp", 0
    )
    middle = (resid_in.astype(jnp.float32) + projected).astype(jnp.bfloat16)
    middle_f32 = middle.astype(jnp.float32)
    normed = middle_f32 * lax.rsqrt(
        jnp.mean(middle_f32 * middle_f32, axis=-1, keepdims=True) + NORM_EPS
    )
    normed = (normed * norm_gain.astype(jnp.float32)).astype(jnp.bfloat16)
    whole_rows = copy_for_each(normed, "tp").reshape(-1, normed.shape[1])
    mixer_out = sent_and_summed(mixer(whole_rows, weights), "tp", 0)
    return (middle_f32 + mixer_out).astype(jnp.bfloat16)


def solution(mesh):
    placed = (
        P(("grp", "sp", "tp"), None),
        P(("grp", "sp"), "tp", None),
        P(("grp", "sp"), "tp", None),
        P(("grp", "sp"), "tp", None),
        P(("grp", "sp"), "tp", None),
        P(("grp", "sp"), "tp", None),
        P(("grp", "sp"), "tp", None),
        P("tp"),
        P("tp"),
        P(),
        P("tp", None),
        P("tp", None),
        P(),
        P("sp", "tp"),
        P("tp", "sp"),
    )
    return jax.shard_map(
        shards, mesh=mesh, in_specs=placed, out_specs=P(("grp", "sp", "tp"), None), check_vma=False
    )
```

```python
import functools
import math

import jax
import jax.numpy as jnp
from jax import lax
from jax.experimental import pallas as pl
from jax.experimental.pallas import tpu as pltpu
from jax.sharding import PartitionSpec as P


NORM_EPS = 1e-06
OUT_SCALE = 0.8
LOG2E = math.log2(math.e)
LAST_DIMS = (((1,), (1,)), ((), ()))
VMEM_LIMIT = 28 * 2**20
EARLY = 8
BATCHES = ()


def split_up(array, dim, peers):
    before, after = (array.shape[:dim], array.shape[dim + 1 :])
    return jnp.moveaxis(array.reshape(*before, peers, -1, *after), dim, 0)


def sent_and_summed(array, axis, dim):
    peers = lax.axis_size(axis)
    parts = lax.all_to_all(split_up(array, dim, peers), axis, 0, 0, tiled=True)
    return jnp.sum(parts.astype(jnp.float32), axis=0)


def after(array, *others):
    return lax.optimization_barrier((array, *others))[0]


def copy_for_each(array, axis):
    copies = jnp.broadcast_to(array, (lax.axis_size(axis), *array.shape))
    return lax.all_to_all(copies, axis, split_axis=0, concat_axis=0, tiled=True)


def ring(block, batches):
    peers = lax.axis_size("sp")
    chips = peers // 2
    onward = [(i, (i + 2) % peers) for i in range(peers)]
    backward = [(i, (i - 2) % peers) for i in range(peers)]
    ahead, behind = block, block
    waiting, stacks, places = [block], [], [0]
    for step in range(1, chips // 2 + 1):
        ahead = lax.ppermute(ahead, "sp", onward)
        waiting.append(ahead)
        places.append(-step % chips)
        if step < chips - chips // 2:
            behind = lax.ppermute(behind, "sp", backward)
            waiting.append(behind)
            places.append(step)
        if step in batches or step == chips // 2:
            stacks.append(stacked(waiting))
            waiting = []
    return stacks, places


def stack_kernel(*refs):
    for i, block in enumerate(refs[:-1]):
        refs[-1][i] = block[...]


def stacked(blocks):
    vmem = pl.BlockSpec(memory_space=pltpu.VMEM)
    return pl.pallas_call(
        stack_kernel,
        in_specs=[vmem] * len(blocks),
        out_specs=vmem,
        out_shape=jax.ShapeDtypeStruct((len(blocks), *blocks[0].shape), blocks[0].dtype),
        compiler_params=pltpu.CompilerParams(vmem_limit_bytes=12 * 2**20),
        name="stack",
    )(*blocks)


def attend_kernel(
    qn_ref, qw_ref, kv_ref, lam_ref, gain_ref, out_ref, q_s, m_s, acc_s, v_s, *, dn, dw, dv, steps, parts
):
    step, part = pl.program_id(0), pl.program_id(1)
    rows = qn_ref.shape[0]
    some = pl.ds(pl.multiple_of(part * (rows // parts), rows // parts), rows // parts)

    @pl.when((step == 0) & (part == 0))
    def _():
        m_s[...] = jnp.full_like(m_s, -jnp.inf)
        acc_s[...] = jnp.zeros_like(acc_s)
        v_s[...] = jnp.ones_like(v_s)
        lane = lax.broadcasted_iota(jnp.int32, (rows, 2 * dn), 1)
        for h in range(2):
            q = qn_ref[:, h * 2 * dn : (h + 1) * 2 * dn]
            for c in range(2):
                keep = (lane < dn) if c == 0 else (lane >= dn)
                q_s[h * 2 + c] = jnp.where(keep, q, jnp.zeros_like(q))
                q_s[4 + h * 2 + c] = qw_ref[:, (h * 2 + c) * dw : (h * 2 + c + 1) * dw]

    at_vn = 2 * dn
    at_kw = at_vn + dv
    at_vw = at_kw + 2 * dw

    @pl.when(part == 0)
    def _():
        v_s[0, :, :dv] = kv_ref[:, at_vn : at_vn + dv]
        v_s[1, :, :dv] = kv_ref[:, at_vw : at_vw + dv]

    for u in range(8):
        wide, c = u >= 4, u % 2
        at = at_kw + c * dw if wide else 0
        width = dw if wide else 2 * dn
        scale = (dw if wide else dn) ** -0.5 * LOG2E
        s = lax.dot_general(
            q_s[u, some], kv_ref[:, at : at + width], LAST_DIMS, preferred_element_type=jnp.float32
        )
        m_old = m_s[u, some]
        m_new = jnp.maximum(m_old, jnp.max(s, axis=1, keepdims=True))
        powers = jnp.exp2((s - m_new) * scale).astype(jnp.bfloat16)
        rescale = jnp.exp2((m_old - m_new) * scale)
        m_s[u, some] = m_new
        acc_s[u, some] = acc_s[u, some] * rescale + jnp.dot(
            powers, v_s[int(wide)], preferred_element_type=jnp.float32
        )

    @pl.when((step == steps - 1) & (part == parts - 1))
    def _():
        for h in range(4):
            first, second = acc_s[2 * h], acc_s[2 * h + 1]
            o = first[:, :dv] / first[:, dv:] - lam_ref[h] * (second[:, :dv] / second[:, dv:])
            square = jnp.mean(o * o, axis=-1, keepdims=True)
            o = o * lax.rsqrt(square + NORM_EPS) * gain_ref[...] * OUT_SCALE
            out_ref[:, h * dv : (h + 1) * dv] = o.astype(out_ref.dtype)


def attention(qn, qw, kv, lam, gain):
    rows = qn.shape[0]
    keys, width = kv.shape
    dv = gain.shape[1]
    dn, dw = qn.shape[1] // 4, qw.shape[1] // 4
    block = math.gcd(keys, 2048)
    steps = keys // block
    return pl.pallas_call(
        functools.partial(attend_kernel, dn=dn, dw=dw, dv=dv, steps=steps, parts=2),
        grid=(steps, 2),
        in_specs=[
            pl.BlockSpec(qn.shape, lambda i, j: (0, 0)),
            pl.BlockSpec(qw.shape, lambda i, j: (0, 0)),
            pl.BlockSpec((block, width), lambda i, j: (i, 0)),
            pl.BlockSpec(memory_space=pltpu.SMEM),
            pl.BlockSpec(gain.shape, lambda i, j: (0, 0)),
        ],
        out_specs=pl.BlockSpec((rows, 4 * dv), lambda i, j: (0, 0)),
        out_shape=jax.ShapeDtypeStruct((rows, 4 * dv), jnp.bfloat16),
        scratch_shapes=[
            pltpu.VMEM((8, rows, 128), jnp.bfloat16),
            pltpu.VMEM((8, rows, 1), jnp.float32),
            pltpu.VMEM((8, rows, 2 * dv), jnp.float32),
            pltpu.VMEM((2, block, 2 * dv), jnp.bfloat16),
        ],
        compiler_params=pltpu.CompilerParams(
            dimension_semantics=("arbitrary", "arbitrary"), vmem_limit_bytes=VMEM_LIMIT
        ),
        cost_estimate=pl.CostEstimate(
            flops=16 * rows * keys * 256, bytes_accessed=keys * width * 2, transcendentals=8 * rows * keys
        ),
        name="attend",
    )(qn, qw, kv, lam, gain)


def early_mixer_kernel(chip_ref, x_ref, *refs, places, batches):
    weights, (out_ref, x_s, out_s) = refs[:-3], refs[-3:]
    chips = len(places)
    each = x_ref.shape[1] // chips

    def columns(at):
        chip = lax.rem(chip_ref[0] + at, chips)
        return pl.ds(pl.multiple_of(chip * each, each), each)

    for i, at in enumerate(places):
        x_s[:, i * each : (i + 1) * each] = x_ref[:, columns(at)]
    for first in range(0, len(weights), batches):
        some = weights[first : first + batches]
        lifted, start = 0.0, 0
        for w in some:
            up = w[:, :, 0].reshape(-1, w.shape[4])
            lifted += jnp.dot(
                x_s[:, start : start + up.shape[0]], up, preferred_element_type=jnp.float32
            )
            start += up.shape[0]
        lifted = jnp.maximum(lifted, 0.0)
        activated = (lifted * lifted).astype(jnp.bfloat16)
        start = 0
        for w in some:
            down = w[:, :, 1].reshape(-1, w.shape[4])
            part = lax.dot_general(
                activated, down, LAST_DIMS, preferred_element_type=jnp.float32
            )
            to = slice(start, start + down.shape[0])
            out_s[:, to] = part if first == 0 else out_s[:, to] + part
            start += down.shape[0]
    for i, at in enumerate(places):
        out_ref[:, columns(at)] = out_s[:, i * each : (i + 1) * each]


def early_mixer(x, weights, places, batches):
    rows, d = x.shape
    half = pl.BlockSpec((rows // 2, d), lambda i: (i, 0))
    hidden = sum(w.shape[4] for w in weights[::batches])
    chip = (lax.axis_index("sp") // 2).astype(jnp.int32).reshape(1)
    return pl.pallas_call(
        functools.partial(early_mixer_kernel, places=places, batches=batches),
        grid=(2,),
        in_specs=[
            pl.BlockSpec(memory_space=pltpu.SMEM),
            half,
            *(pl.BlockSpec(memory_space=pltpu.VMEM) for _ in weights),
        ],
        out_specs=half,
        out_shape=jax.ShapeDtypeStruct((rows, d), jnp.float32),
        scratch_shapes=[
            pltpu.VMEM((rows // 2, d), jnp.bfloat16),
            pltpu.VMEM((rows // 2, d), jnp.float32),
        ],
        compiler_params=pltpu.CompilerParams(
            dimension_semantics=("arbitrary",), vmem_limit_bytes=30 * 2**20
        ),
        cost_estimate=pl.CostEstimate(
            flops=4 * rows * d * hidden, bytes_accessed=4 * d * hidden, transcendentals=0
        ),
        name="early_mixer",
    )(chip, x, *weights)


def mixer_kernel(x_ref, w_ref, early_ref, out_ref, lifted, activated, *, half):
    step = pl.program_id(0)
    depth = w_ref.shape[0] * w_ref.shape[2]
    w = w_ref[...].reshape(depth, w_ref.shape[3])

    @pl.when(step < half)
    def _():
        at = pl.multiple_of(step * depth, depth)
        part = jnp.dot(x_ref[:, pl.ds(at, depth)], w, preferred_element_type=jnp.float32)

        @pl.when(step == 0)
        def _():
            lifted[...] = part

        @pl.when(step > 0)
        def _():
            lifted[...] += part

    @pl.when(step == half - 1)
    def _():
        up = jnp.maximum(lifted[...], 0.0)
        activated[...] = (up * up).astype(jnp.bfloat16)

    @pl.when(step >= half)
    def _():
        part = lax.dot_general(activated[...], w, LAST_DIMS, preferred_element_type=jnp.float32)
        out_ref[...] = (early_ref[...] + part).astype(jnp.bfloat16)


def mixer(x, w, early):
    rows, d = x.shape
    shards, _, each, hidden = w.shape
    group = math.gcd(shards, 8)
    half = shards // group
    depth = group * each
    return pl.pallas_call(
        functools.partial(mixer_kernel, half=half),
        grid=(2 * half,),
        in_specs=[
            pl.BlockSpec((rows, d), lambda i: (0, 0)),
            pl.BlockSpec((group, 1, each, hidden), lambda i: (i % half, i // half, 0, 0)),
            pl.BlockSpec((rows, depth), lambda i: (0, jnp.maximum(i - half, 0))),
        ],
        out_specs=pl.BlockSpec((rows, depth), lambda i: (0, jnp.maximum(i - half, 0))),
        out_shape=jax.ShapeDtypeStruct((rows, d), jnp.bfloat16),
        scratch_shapes=[
            pltpu.VMEM((rows, hidden), jnp.float32),
            pltpu.VMEM((rows, hidden), jnp.bfloat16),
        ],
        compiler_params=pltpu.CompilerParams(
            dimension_semantics=("arbitrary",), vmem_limit_bytes=20 * 2**20
        ),
        cost_estimate=pl.CostEstimate(
            flops=4 * rows * d * hidden, bytes_accessed=4 * d * hidden, transcendentals=0
        ),
        name="mixer",
    )(x, w, early)


def shards(
    resid_in,
    query_narrow,
    key_narrow,
    value_narrow,
    query_wide,
    key_wide,
    value_wide,
    lambda_narrow,
    lambda_wide,
    head_gain,
    out_narrow,
    out_wide,
    norm_gain,
    up_weight,
    down_weight,
):
    rows = query_narrow.shape[0]
    sp, grp = lax.axis_size("sp"), lax.axis_size("grp")
    core, side = lax.axis_index("sp") % 2, lax.axis_index("grp") % 2
    other_core = [(i, i ^ 1) for i in range(sp)]
    other_group = [(i, i ^ 1) for i in range(grp)]
    own = jnp.concatenate(
        [a.reshape(rows, -1) for a in (key_narrow, value_narrow, key_wide, value_wide)], axis=1
    )
    kv = lax.all_gather(own, "sp", axis=0, tiled=True)
    own_weights = jnp.stack([up_weight, down_weight.T])
    hidden = up_weight.shape[1]
    share = hidden * EARLY // 16
    each = share // 4
    late_weights = lax.all_gather(own_weights[:, :, share:], "sp", axis=0, tiled=False)
    mine = lax.dynamic_slice_in_dim(own_weights, (2 * side + core) * each, each, 2)
    theirs = lax.dynamic_slice_in_dim(own_weights, (2 * side + 1 - core) * each, each, 2)
    theirs = lax.ppermute(theirs, "sp", other_core)
    chip = jnp.where(core == 0, jnp.stack([mine, theirs]), jnp.stack([theirs, mine]))
    stacks, places = ring(chip, BATCHES)
    early_weights = [[], [], [], []]
    for stack in stacks:
        swapped = lax.ppermute(stack, "grp", other_group)
        first = lax.ppermute(stack, "sp", other_core)
        second = lax.ppermute(swapped, "sp", other_core)
        for kind, array in zip(early_weights, (stack, first, swapped, second)):
            kind.append(array)
    kv = after(kv, *stacks)
    attended = attention(
        query_narrow.reshape(rows, -1),
        query_wide.reshape(rows, -1),
        kv,
        jnp.concatenate([lambda_narrow, lambda_wide]),
        head_gain.reshape(1, -1),
    )
    out_rows = jnp.concatenate([out_narrow, out_wide], axis=0)
    projected = jnp.dot(attended, out_rows, preferred_element_type=jnp.float32)
    projected = sent_and_summed(projected.astype(jnp.bfloat16), "tp", 0)
    middle = (resid_in.astype(jnp.float32) + projected).astype(jnp.bfloat16)
    middle_f32 = middle.astype(jnp.float32)
    normed = middle_f32 * lax.rsqrt(
        jnp.mean(middle_f32 * middle_f32, axis=-1, keepdims=True) + NORM_EPS
    )
    normed = (normed * norm_gain.astype(jnp.float32)).astype(jnp.bfloat16)
    normed = copy_for_each(normed, "tp").reshape(-1, normed.shape[1])
    early = early_mixer(normed, sum(early_weights, []), places, len(stacks))
    mixer_out = sent_and_summed(mixer(normed, late_weights, early), "tp", 0)
    return (middle_f32 + mixer_out).astype(jnp.bfloat16)


def solution(mesh):
    placed = (
        P(("grp", "sp", "tp"), None),
        P(("grp", "sp"), "tp", None),
        P(("grp", "sp"), "tp", None),
        P(("grp", "sp"), "tp", None),
        P(("grp", "sp"), "tp", None),
        P(("grp", "sp"), "tp", None),
        P(("grp", "sp"), "tp", None),
        P("tp"),
        P("tp"),
        P(),
        P("tp", None),
        P("tp", None),
        P(),
        P("sp", "tp"),
        P("tp", "sp"),
    )
    return jax.shard_map(
        shards, mesh=mesh, in_specs=placed, out_specs=P(("grp", "sp", "tp"), None), check_vma=False
    )
```

```python
import functools
import math

import jax
import jax.numpy as jnp
from jax import lax
from jax.experimental import pallas as pl
from jax.experimental.pallas import tpu as pltpu
from jax.sharding import PartitionSpec as P


NORM_EPS = 1e-06
OUT_SCALE = 0.8
LOG2E = math.log2(math.e)
LAST_DIMS = (((1,), (1,)), ((), ()))
VMEM_LIMIT = 58 * 2**20
EARLY = 8
BATCHES = ()


def split_up(array, dim, peers):
    before, after = (array.shape[:dim], array.shape[dim + 1 :])
    return jnp.moveaxis(array.reshape(*before, peers, -1, *after), dim, 0)


def sent_and_summed(array, axis, dim):
    peers = lax.axis_size(axis)
    parts = lax.all_to_all(split_up(array, dim, peers), axis, 0, 0, tiled=True)
    return jnp.sum(parts.astype(jnp.float32), axis=0)


def after(array, *others):
    return lax.optimization_barrier((array, *others))[0]


def copy_for_each(array, axis):
    copies = jnp.broadcast_to(array, (lax.axis_size(axis), *array.shape))
    return lax.all_to_all(copies, axis, split_axis=0, concat_axis=0, tiled=True)


def ring(block, batches):
    peers = lax.axis_size("sp")
    chips = peers // 2
    onward = [(i, (i + 2) % peers) for i in range(peers)]
    backward = [(i, (i - 2) % peers) for i in range(peers)]
    ahead, behind = block, block
    waiting, stacks, places = [block], [], [0]
    for step in range(1, chips // 2 + 1):
        ahead = lax.ppermute(ahead, "sp", onward)
        waiting.append(ahead)
        places.append(-step % chips)
        if step < chips - chips // 2:
            behind = lax.ppermute(behind, "sp", backward)
            waiting.append(behind)
            places.append(step)
        if step in batches or step == chips // 2:
            stacks.append(stacked(waiting))
            waiting = []
    return stacks, places


def stack_kernel(*refs):
    for i, block in enumerate(refs[:-1]):
        refs[-1][i] = block[...]


def stacked(blocks):
    vmem = pl.BlockSpec(memory_space=pltpu.VMEM)
    return pl.pallas_call(
        stack_kernel,
        in_specs=[vmem] * len(blocks),
        out_specs=vmem,
        out_shape=jax.ShapeDtypeStruct((len(blocks), *blocks[0].shape), blocks[0].dtype),
        compiler_params=pltpu.CompilerParams(vmem_limit_bytes=12 * 2**20),
        name="stack",
    )(*blocks)


def attend_kernel(
    qn_ref, qw_ref, kv_ref, lam_ref, gain_ref, out_ref, q_s, m_s, acc_s, v_s, *, dn, dw, dv, steps, parts
):
    step, part = pl.program_id(0), pl.program_id(1)
    rows = qn_ref.shape[0]
    some = pl.ds(pl.multiple_of(part * (rows // parts), rows // parts), rows // parts)

    @pl.when((step == 0) & (part == 0))
    def _():
        m_s[...] = jnp.full_like(m_s, -jnp.inf)
        acc_s[...] = jnp.zeros_like(acc_s)
        v_s[...] = jnp.ones_like(v_s)
        lane = lax.broadcasted_iota(jnp.int32, (rows, 2 * dn), 1)
        for h in range(2):
            q = qn_ref[:, h * 2 * dn : (h + 1) * 2 * dn]
            for c in range(2):
                keep = (lane < dn) if c == 0 else (lane >= dn)
                q_s[h * 2 + c] = jnp.where(keep, q, jnp.zeros_like(q))
                q_s[4 + h * 2 + c] = qw_ref[:, (h * 2 + c) * dw : (h * 2 + c + 1) * dw]

    at_vn = 2 * dn
    at_kw = at_vn + dv
    at_vw = at_kw + 2 * dw

    @pl.when(part == 0)
    def _():
        v_s[0, :, :dv] = kv_ref[:, at_vn : at_vn + dv]
        v_s[1, :, :dv] = kv_ref[:, at_vw : at_vw + dv]

    for u in range(8):
        wide, c = u >= 4, u % 2
        at = at_kw + c * dw if wide else 0
        width = dw if wide else 2 * dn
        scale = (dw if wide else dn) ** -0.5 * LOG2E
        s = lax.dot_general(
            q_s[u, some], kv_ref[:, at : at + width], LAST_DIMS, preferred_element_type=jnp.float32
        )
        m_old = m_s[u, some]
        m_new = jnp.maximum(m_old, jnp.max(s, axis=1, keepdims=True))
        powers = jnp.exp2((s - m_new) * scale).astype(jnp.bfloat16)
        rescale = jnp.exp2((m_old - m_new) * scale)
        m_s[u, some] = m_new
        acc_s[u, some] = acc_s[u, some] * rescale + jnp.dot(
            powers, v_s[int(wide)], preferred_element_type=jnp.float32
        )

    @pl.when((step == steps - 1) & (part == parts - 1))
    def _():
        for h in range(4):
            first, second = acc_s[2 * h], acc_s[2 * h + 1]
            o = first[:, :dv] / first[:, dv:] - lam_ref[h] * (second[:, :dv] / second[:, dv:])
            square = jnp.mean(o * o, axis=-1, keepdims=True)
            o = o * lax.rsqrt(square + NORM_EPS) * gain_ref[...] * OUT_SCALE
            out_ref[:, h * dv : (h + 1) * dv] = o.astype(out_ref.dtype)


def attention(qn, qw, kv, lam, gain):
    rows = qn.shape[0]
    keys, width = kv.shape
    dv = gain.shape[1]
    dn, dw = qn.shape[1] // 4, qw.shape[1] // 4
    block = math.gcd(keys, 2048)
    steps = keys // block
    return pl.pallas_call(
        functools.partial(attend_kernel, dn=dn, dw=dw, dv=dv, steps=steps, parts=1),
        grid=(steps, 1),
        in_specs=[
            pl.BlockSpec(qn.shape, lambda i, j: (0, 0)),
            pl.BlockSpec(qw.shape, lambda i, j: (0, 0)),
            pl.BlockSpec((block, width), lambda i, j: (i, 0)),
            pl.BlockSpec(memory_space=pltpu.SMEM),
            pl.BlockSpec(gain.shape, lambda i, j: (0, 0)),
        ],
        out_specs=pl.BlockSpec((rows, 4 * dv), lambda i, j: (0, 0)),
        out_shape=jax.ShapeDtypeStruct((rows, 4 * dv), jnp.bfloat16),
        scratch_shapes=[
            pltpu.VMEM((8, rows, 128), jnp.bfloat16),
            pltpu.VMEM((8, rows, 1), jnp.float32),
            pltpu.VMEM((8, rows, 2 * dv), jnp.float32),
            pltpu.VMEM((2, block, 2 * dv), jnp.bfloat16),
        ],
        compiler_params=pltpu.CompilerParams(
            dimension_semantics=("arbitrary", "arbitrary"), vmem_limit_bytes=VMEM_LIMIT
        ),
        cost_estimate=pl.CostEstimate(
            flops=16 * rows * keys * 256, bytes_accessed=keys * width * 2, transcendentals=8 * rows * keys
        ),
        name="attend",
    )(qn, qw, kv, lam, gain)


def early_mixer_kernel(chip_ref, x_ref, *refs, places, batches):
    weights, (out_ref, x_s, out_s) = refs[:-3], refs[-3:]
    chips = len(places)
    each = x_ref.shape[1] // chips

    def columns(at):
        chip = lax.rem(chip_ref[0] + at, chips)
        return pl.ds(pl.multiple_of(chip * each, each), each)

    for i, at in enumerate(places):
        x_s[:, i * each : (i + 1) * each] = x_ref[:, columns(at)]
    for first in range(0, len(weights), batches):
        some = weights[first : first + batches]
        lifted, start = 0.0, 0
        for w in some:
            up = w[:, :, 0].reshape(-1, w.shape[4])
            lifted += jnp.dot(
                x_s[:, start : start + up.shape[0]], up, preferred_element_type=jnp.float32
            )
            start += up.shape[0]
        lifted = jnp.maximum(lifted, 0.0)
        activated = (lifted * lifted).astype(jnp.bfloat16)
        start = 0
        for w in some:
            down = w[:, :, 1].reshape(-1, w.shape[4])
            part = lax.dot_general(
                activated, down, LAST_DIMS, preferred_element_type=jnp.float32
            )
            to = slice(start, start + down.shape[0])
            out_s[:, to] = part if first == 0 else out_s[:, to] + part
            start += down.shape[0]
    for i, at in enumerate(places):
        out_ref[:, columns(at)] = out_s[:, i * each : (i + 1) * each]


def early_mixer(x, weights, places, batches):
    rows, d = x.shape
    half = pl.BlockSpec((rows // 2, d), lambda i: (i, 0))
    hidden = sum(w.shape[4] for w in weights[::batches])
    chip = (lax.axis_index("sp") // 2).astype(jnp.int32).reshape(1)
    return pl.pallas_call(
        functools.partial(early_mixer_kernel, places=places, batches=batches),
        grid=(2,),
        in_specs=[
            pl.BlockSpec(memory_space=pltpu.SMEM),
            half,
            *(pl.BlockSpec(memory_space=pltpu.VMEM) for _ in weights),
        ],
        out_specs=half,
        out_shape=jax.ShapeDtypeStruct((rows, d), jnp.float32),
        scratch_shapes=[
            pltpu.VMEM((rows // 2, d), jnp.bfloat16),
            pltpu.VMEM((rows // 2, d), jnp.float32),
        ],
        compiler_params=pltpu.CompilerParams(
            dimension_semantics=("arbitrary",), vmem_limit_bytes=50 * 2**20
        ),
        cost_estimate=pl.CostEstimate(
            flops=4 * rows * d * hidden, bytes_accessed=4 * d * hidden, transcendentals=0
        ),
        name="early_mixer",
    )(chip, x, *weights)


def mixer_kernel(x_ref, w_ref, early_ref, out_ref, lifted, activated, *, half):
    step = pl.program_id(0)
    depth = w_ref.shape[0] * w_ref.shape[2]
    w = w_ref[...].reshape(depth, w_ref.shape[3])

    @pl.when(step < half)
    def _():
        at = pl.multiple_of(step * depth, depth)
        part = jnp.dot(x_ref[:, pl.ds(at, depth)], w, preferred_element_type=jnp.float32)

        @pl.when(step == 0)
        def _():
            lifted[...] = part

        @pl.when(step > 0)
        def _():
            lifted[...] += part

    @pl.when(step == half - 1)
    def _():
        up = jnp.maximum(lifted[...], 0.0)
        activated[...] = (up * up).astype(jnp.bfloat16)

    @pl.when(step >= half)
    def _():
        part = lax.dot_general(activated[...], w, LAST_DIMS, preferred_element_type=jnp.float32)
        out_ref[...] = (early_ref[...] + part).astype(jnp.bfloat16)


def mixer(x, w, early):
    rows, d = x.shape
    shards, _, each, hidden = w.shape
    group = math.gcd(shards, 8)
    half = shards // group
    depth = group * each
    return pl.pallas_call(
        functools.partial(mixer_kernel, half=half),
        grid=(2 * half,),
        in_specs=[
            pl.BlockSpec((rows, d), lambda i: (0, 0)),
            pl.BlockSpec((group, 1, each, hidden), lambda i: (i % half, i // half, 0, 0)),
            pl.BlockSpec((rows, depth), lambda i: (0, jnp.maximum(i - half, 0))),
        ],
        out_specs=pl.BlockSpec((rows, depth), lambda i: (0, jnp.maximum(i - half, 0))),
        out_shape=jax.ShapeDtypeStruct((rows, d), jnp.bfloat16),
        scratch_shapes=[
            pltpu.VMEM((rows, hidden), jnp.float32),
            pltpu.VMEM((rows, hidden), jnp.bfloat16),
        ],
        compiler_params=pltpu.CompilerParams(
            dimension_semantics=("arbitrary",), vmem_limit_bytes=50 * 2**20
        ),
        cost_estimate=pl.CostEstimate(
            flops=4 * rows * d * hidden, bytes_accessed=4 * d * hidden, transcendentals=0
        ),
        name="mixer",
    )(x, w, early)


def shards(
    resid_in,
    query_narrow,
    key_narrow,
    value_narrow,
    query_wide,
    key_wide,
    value_wide,
    lambda_narrow,
    lambda_wide,
    head_gain,
    out_narrow,
    out_wide,
    norm_gain,
    up_weight,
    down_weight,
):
    rows = query_narrow.shape[0]
    sp, grp = lax.axis_size("sp"), lax.axis_size("grp")
    core, side = lax.axis_index("sp") % 2, lax.axis_index("grp") % 2
    other_core = [(i, i ^ 1) for i in range(sp)]
    other_group = [(i, i ^ 1) for i in range(grp)]
    own = jnp.concatenate(
        [a.reshape(rows, -1) for a in (key_narrow, value_narrow, key_wide, value_wide)], axis=1
    )
    kv = lax.all_gather(own, "sp", axis=0, tiled=True)
    own_weights = jnp.stack([up_weight, down_weight.T])
    hidden = up_weight.shape[1]
    share = hidden * EARLY // 16
    each = share // 4
    late_weights = lax.all_gather(own_weights[:, :, share:], "sp", axis=0, tiled=False)
    mine = lax.dynamic_slice_in_dim(own_weights, (2 * side + core) * each, each, 2)
    theirs = lax.dynamic_slice_in_dim(own_weights, (2 * side + 1 - core) * each, each, 2)
    theirs = lax.ppermute(theirs, "sp", other_core)
    chip = jnp.where(core == 0, jnp.stack([mine, theirs]), jnp.stack([theirs, mine]))
    stacks, places = ring(chip, BATCHES)
    early_weights = [[], [], [], []]
    for stack in stacks:
        swapped = lax.ppermute(stack, "grp", other_group)
        first = lax.ppermute(stack, "sp", other_core)
        second = lax.ppermute(swapped, "sp", other_core)
        for kind, array in zip(early_weights, (stack, first, swapped, second)):
            kind.append(array)
    kv = after(kv, *stacks)
    attended = attention(
        query_narrow.reshape(rows, -1),
        query_wide.reshape(rows, -1),
        kv,
        jnp.concatenate([lambda_narrow, lambda_wide]),
        head_gain.reshape(1, -1),
    )
    out_rows = jnp.concatenate([out_narrow, out_wide], axis=0)
    projected = jnp.dot(attended, out_rows, preferred_element_type=jnp.float32)
    projected = sent_and_summed(projected.astype(jnp.bfloat16), "tp", 0)
    middle = (resid_in.astype(jnp.float32) + projected).astype(jnp.bfloat16)
    middle_f32 = middle.astype(jnp.float32)
    normed = middle_f32 * lax.rsqrt(
        jnp.mean(middle_f32 * middle_f32, axis=-1, keepdims=True) + NORM_EPS
    )
    normed = (normed * norm_gain.astype(jnp.float32)).astype(jnp.bfloat16)
    normed = copy_for_each(normed, "tp").reshape(-1, normed.shape[1])
    early = early_mixer(normed, sum(early_weights, []), places, len(stacks))
    mixer_out = sent_and_summed(mixer(normed, late_weights, early), "tp", 0)
    return (middle_f32 + mixer_out).astype(jnp.bfloat16)


def solution(mesh):
    placed = (
        P(("grp", "sp", "tp"), None),
        P(("grp", "sp"), "tp", None),
        P(("grp", "sp"), "tp", None),
        P(("grp", "sp"), "tp", None),
        P(("grp", "sp"), "tp", None),
        P(("grp", "sp"), "tp", None),
        P(("grp", "sp"), "tp", None),
        P("tp"),
        P("tp"),
        P(),
        P("tp", None),
        P("tp", None),
        P(),
        P("sp", "tp"),
        P("tp", "sp"),
    )
    return jax.shard_map(
        shards, mesh=mesh, in_specs=placed, out_specs=P(("grp", "sp", "tp"), None), check_vma=False
    )
```

```python
import functools
import math

import jax
import jax.numpy as jnp
from jax import lax
from jax.experimental import pallas as pl
from jax.experimental.pallas import tpu as pltpu
from jax.sharding import PartitionSpec as P


NORM_EPS = 1e-06
OUT_SCALE = 0.8
LOG2E = math.log2(math.e)
LAST_DIMS = (((1,), (1,)), ((), ()))
VMEM_LIMIT = 58 * 2**20
EARLY = 8


def split_up(array, dim, peers):
    before, after = (array.shape[:dim], array.shape[dim + 1 :])
    return jnp.moveaxis(array.reshape(*before, peers, -1, *after), dim, 0)


def sent_and_summed(array, axis, dim):
    peers = lax.axis_size(axis)
    parts = lax.all_to_all(split_up(array, dim, peers), axis, 0, 0, tiled=True)
    return jnp.sum(parts.astype(jnp.float32), axis=0)


def after(array, *others):
    return lax.optimization_barrier((array, *others))[0]


def copy_for_each(array, axis):
    copies = jnp.broadcast_to(array, (lax.axis_size(axis), *array.shape))
    return lax.all_to_all(copies, axis, split_axis=0, concat_axis=0, tiled=True)


def ring(block):
    peers = lax.axis_size("sp")
    chips = peers // 2
    onward = [(i, (i + 2) % peers) for i in range(peers)]
    backward = [(i, (i - 2) % peers) for i in range(peers)]
    ahead, behind = block, block
    blocks, places = [block], [0]
    for step in range(1, chips // 2 + 1):
        ahead = lax.ppermute(ahead, "sp", onward)
        blocks.append(ahead)
        places.append(-step % chips)
        if step < chips - chips // 2:
            behind = lax.ppermute(behind, "sp", backward)
            blocks.append(behind)
            places.append(step)
    return stacked(blocks), places


def stack_kernel(*refs):
    for i, block in enumerate(refs[:-1]):
        refs[-1][i] = block[...]


def stacked(blocks):
    vmem = pl.BlockSpec(memory_space=pltpu.VMEM)
    return pl.pallas_call(
        stack_kernel,
        in_specs=[vmem] * len(blocks),
        out_specs=vmem,
        out_shape=jax.ShapeDtypeStruct((len(blocks), *blocks[0].shape), blocks[0].dtype),
        compiler_params=pltpu.CompilerParams(vmem_limit_bytes=12 * 2**20),
        name="stack",
    )(*blocks)


def attend_kernel(
    qn_ref, qw_ref, kv_ref, lam_ref, gain_ref, out_ref, q_s, m_s, acc_s, v_s, *, dn, dw, dv, steps, parts
):
    step, part = pl.program_id(0), pl.program_id(1)
    rows = qn_ref.shape[0]
    some = pl.ds(pl.multiple_of(part * (rows // parts), rows // parts), rows // parts)

    @pl.when((step == 0) & (part == 0))
    def _():
        m_s[...] = jnp.full_like(m_s, -jnp.inf)
        acc_s[...] = jnp.zeros_like(acc_s)
        v_s[...] = jnp.ones_like(v_s)
        lane = lax.broadcasted_iota(jnp.int32, (rows, 2 * dn), 1)
        for h in range(2):
            q = qn_ref[:, h * 2 * dn : (h + 1) * 2 * dn]
            for c in range(2):
                keep = (lane < dn) if c == 0 else (lane >= dn)
                q_s[h * 2 + c] = jnp.where(keep, q, jnp.zeros_like(q))
                q_s[4 + h * 2 + c] = qw_ref[:, (h * 2 + c) * dw : (h * 2 + c + 1) * dw]

    at_vn = 2 * dn
    at_kw = at_vn + dv
    at_vw = at_kw + 2 * dw

    @pl.when(part == 0)
    def _():
        v_s[0, :, :dv] = kv_ref[:, at_vn : at_vn + dv]
        v_s[1, :, :dv] = kv_ref[:, at_vw : at_vw + dv]

    for u in range(8):
        wide, c = u >= 4, u % 2
        at = at_kw + c * dw if wide else 0
        width = dw if wide else 2 * dn
        scale = (dw if wide else dn) ** -0.5 * LOG2E
        s = lax.dot_general(
            q_s[u, some], kv_ref[:, at : at + width], LAST_DIMS, preferred_element_type=jnp.float32
        )
        m_old = m_s[u, some]
        m_new = jnp.maximum(m_old, jnp.max(s, axis=1, keepdims=True))
        powers = jnp.exp2((s - m_new) * scale).astype(jnp.bfloat16)
        rescale = jnp.exp2((m_old - m_new) * scale)
        m_s[u, some] = m_new
        acc_s[u, some] = acc_s[u, some] * rescale + jnp.dot(
            powers, v_s[int(wide)], preferred_element_type=jnp.float32
        )

    @pl.when((step == steps - 1) & (part == parts - 1))
    def _():
        for h in range(4):
            first, second = acc_s[2 * h], acc_s[2 * h + 1]
            o = first[:, :dv] / first[:, dv:] - lam_ref[h] * (second[:, :dv] / second[:, dv:])
            square = jnp.mean(o * o, axis=-1, keepdims=True)
            o = o * lax.rsqrt(square + NORM_EPS) * gain_ref[...] * OUT_SCALE
            out_ref[:, h * dv : (h + 1) * dv] = o.astype(out_ref.dtype)


def attention(qn, qw, kv, lam, gain):
    rows = qn.shape[0]
    keys, width = kv.shape
    dv = gain.shape[1]
    dn, dw = qn.shape[1] // 4, qw.shape[1] // 4
    block = math.gcd(keys, 2048)
    steps = keys // block
    return pl.pallas_call(
        functools.partial(attend_kernel, dn=dn, dw=dw, dv=dv, steps=steps, parts=1),
        grid=(steps, 1),
        in_specs=[
            pl.BlockSpec(qn.shape, lambda i, j: (0, 0)),
            pl.BlockSpec(qw.shape, lambda i, j: (0, 0)),
            pl.BlockSpec((block, width), lambda i, j: (i, 0)),
            pl.BlockSpec(memory_space=pltpu.SMEM),
            pl.BlockSpec(gain.shape, lambda i, j: (0, 0)),
        ],
        out_specs=pl.BlockSpec((rows, 4 * dv), lambda i, j: (0, 0)),
        out_shape=jax.ShapeDtypeStruct((rows, 4 * dv), jnp.bfloat16),
        scratch_shapes=[
            pltpu.VMEM((8, rows, 128), jnp.bfloat16),
            pltpu.VMEM((8, rows, 1), jnp.float32),
            pltpu.VMEM((8, rows, 2 * dv), jnp.float32),
            pltpu.VMEM((2, block, 2 * dv), jnp.bfloat16),
        ],
        compiler_params=pltpu.CompilerParams(
            dimension_semantics=("arbitrary", "arbitrary"), vmem_limit_bytes=VMEM_LIMIT
        ),
        cost_estimate=pl.CostEstimate(
            flops=16 * rows * keys * 256, bytes_accessed=keys * width * 2, transcendentals=8 * rows * keys
        ),
        name="attend",
    )(qn, qw, kv, lam, gain)


def early_mixer_kernel(chip_ref, x_ref, *refs, places):
    arrays, (out_ref, w_s, x_s, out_s, sem) = refs[:-5], refs[-5:]
    chips = len(places)
    each = x_ref.shape[1] // chips
    copies = [pltpu.make_async_copy(w, w_s.at[i], sem.at[i]) for i, w in enumerate(arrays)]
    for copy in copies:
        copy.start()

    def columns(at):
        chip = lax.rem(chip_ref[0] + at, chips)
        return pl.ds(pl.multiple_of(chip * each, each), each)

    for i, at in enumerate(places):
        x_s[:, i * each : (i + 1) * each] = x_ref[:, columns(at)]
    for k, copy in enumerate(copies):
        copy.wait()
        up = w_s[k, :, :, 0].reshape(x_ref.shape[1], w_s.shape[5])
        down = w_s[k, :, :, 1].reshape(x_ref.shape[1], w_s.shape[5])
        lifted = jnp.maximum(jnp.dot(x_s[...], up, preferred_element_type=jnp.float32), 0.0)
        part = lax.dot_general(
            (lifted * lifted).astype(jnp.bfloat16),
            down,
            LAST_DIMS,
            preferred_element_type=jnp.float32,
        )
        out_s[...] = part if k == 0 else out_s[...] + part
    for i, at in enumerate(places):
        out_ref[:, columns(at)] = out_s[:, i * each : (i + 1) * each]


def early_mixer(x, weights, places):
    rows, d = x.shape
    hidden = sum(w.shape[4] for w in weights)
    chip = (lax.axis_index("sp") // 2).astype(jnp.int32).reshape(1)
    vmem = pl.BlockSpec(memory_space=pltpu.VMEM)
    return pl.pallas_call(
        functools.partial(early_mixer_kernel, places=places),
        in_specs=[
            pl.BlockSpec(memory_space=pltpu.SMEM),
            vmem,
            *(pl.BlockSpec(memory_space=pl.ANY) for _ in weights),
        ],
        out_specs=vmem,
        out_shape=jax.ShapeDtypeStruct((rows, d), jnp.float32),
        scratch_shapes=[
            pltpu.VMEM((len(weights), *weights[0].shape), weights[0].dtype),
            pltpu.VMEM((rows, d), jnp.bfloat16),
            pltpu.VMEM((rows, d), jnp.float32),
            pltpu.SemaphoreType.DMA((len(weights),)),
        ],
        compiler_params=pltpu.CompilerParams(vmem_limit_bytes=50 * 2**20),
        cost_estimate=pl.CostEstimate(
            flops=4 * rows * d * hidden, bytes_accessed=4 * d * hidden, transcendentals=0
        ),
        name="early_mixer",
    )(chip, x, *weights)


def mixer_kernel(x_ref, w_ref, early_ref, out_ref, lifted, activated, *, half):
    step = pl.program_id(0)
    depth = w_ref.shape[0] * w_ref.shape[2]
    w = w_ref[...].reshape(depth, w_ref.shape[3])

    @pl.when(step < half)
    def _():
        at = pl.multiple_of(step * depth, depth)
        part = jnp.dot(x_ref[:, pl.ds(at, depth)], w, preferred_element_type=jnp.float32)

        @pl.when(step == 0)
        def _():
            lifted[...] = part

        @pl.when(step > 0)
        def _():
            lifted[...] += part

    @pl.when(step == half - 1)
    def _():
        up = jnp.maximum(lifted[...], 0.0)
        activated[...] = (up * up).astype(jnp.bfloat16)

    @pl.when(step >= half)
    def _():
        part = lax.dot_general(activated[...], w, LAST_DIMS, preferred_element_type=jnp.float32)
        out_ref[...] = (early_ref[...] + part).astype(jnp.bfloat16)


def mixer(x, w, early):
    rows, d = x.shape
    shards, _, each, hidden = w.shape
    group = math.gcd(shards, 32)
    half = shards // group
    depth = group * each
    return pl.pallas_call(
        functools.partial(mixer_kernel, half=half),
        grid=(2 * half,),
        in_specs=[
            pl.BlockSpec((rows, d), lambda i: (0, 0)),
            pl.BlockSpec((group, 1, each, hidden), lambda i: (i % half, i // half, 0, 0)),
            pl.BlockSpec((rows, depth), lambda i: (0, jnp.maximum(i - half, 0))),
        ],
        out_specs=pl.BlockSpec((rows, depth), lambda i: (0, jnp.maximum(i - half, 0))),
        out_shape=jax.ShapeDtypeStruct((rows, d), jnp.bfloat16),
        scratch_shapes=[
            pltpu.VMEM((rows, hidden), jnp.float32),
            pltpu.VMEM((rows, hidden), jnp.bfloat16),
        ],
        compiler_params=pltpu.CompilerParams(
            dimension_semantics=("arbitrary",), vmem_limit_bytes=50 * 2**20
        ),
        cost_estimate=pl.CostEstimate(
            flops=4 * rows * d * hidden, bytes_accessed=4 * d * hidden, transcendentals=0
        ),
        name="mixer",
    )(x, w, early)


def shards(
    resid_in,
    query_narrow,
    key_narrow,
    value_narrow,
    query_wide,
    key_wide,
    value_wide,
    lambda_narrow,
    lambda_wide,
    head_gain,
    out_narrow,
    out_wide,
    norm_gain,
    up_weight,
    down_weight,
):
    rows = query_narrow.shape[0]
    sp, grp = lax.axis_size("sp"), lax.axis_size("grp")
    core, side = lax.axis_index("sp") % 2, lax.axis_index("grp") % 2
    other_core = [(i, i ^ 1) for i in range(sp)]
    other_group = [(i, i ^ 1) for i in range(grp)]
    own = jnp.concatenate(
        [a.reshape(rows, -1) for a in (key_narrow, value_narrow, key_wide, value_wide)], axis=1
    )
    kv = lax.all_gather(own, "sp", axis=0, tiled=True)
    own_weights = jnp.stack([up_weight, down_weight.T])
    hidden = up_weight.shape[1]
    share = hidden * EARLY // 16
    each = share // 4
    late_weights = lax.all_gather(own_weights[:, :, share:], "sp", axis=0, tiled=False)
    mine = lax.dynamic_slice_in_dim(own_weights, (2 * side + core) * each, each, 2)
    theirs = lax.dynamic_slice_in_dim(own_weights, (2 * side + 1 - core) * each, each, 2)
    theirs = lax.ppermute(theirs, "sp", other_core)
    chip = jnp.where(core == 0, jnp.stack([mine, theirs]), jnp.stack([theirs, mine]))
    stack, places = ring(chip)
    swapped = lax.ppermute(stack, "grp", other_group)
    first = lax.ppermute(stack, "sp", other_core)
    second = lax.ppermute(swapped, "sp", other_core)
    early_weights = (stack, first, swapped, second)
    kv = after(kv, stack)
    attended = attention(
        query_narrow.reshape(rows, -1),
        query_wide.reshape(rows, -1),
        kv,
        jnp.concatenate([lambda_narrow, lambda_wide]),
        head_gain.reshape(1, -1),
    )
    out_rows = jnp.concatenate([out_narrow, out_wide], axis=0)
    projected = jnp.dot(attended, out_rows, preferred_element_type=jnp.float32)
    projected = sent_and_summed(projected.astype(jnp.bfloat16), "tp", 0)
    middle = (resid_in.astype(jnp.float32) + projected).astype(jnp.bfloat16)
    middle_f32 = middle.astype(jnp.float32)
    normed = middle_f32 * lax.rsqrt(
        jnp.mean(middle_f32 * middle_f32, axis=-1, keepdims=True) + NORM_EPS
    )
    normed = (normed * norm_gain.astype(jnp.float32)).astype(jnp.bfloat16)
    normed = copy_for_each(normed, "tp").reshape(-1, normed.shape[1])
    early = early_mixer(normed, early_weights, places)
    mixer_out = sent_and_summed(mixer(normed, late_weights, early), "tp", 0)
    return (middle_f32 + mixer_out).astype(jnp.bfloat16)


def solution(mesh):
    placed = (
        P(("grp", "sp", "tp"), None),
        P(("grp", "sp"), "tp", None),
        P(("grp", "sp"), "tp", None),
        P(("grp", "sp"), "tp", None),
        P(("grp", "sp"), "tp", None),
        P(("grp", "sp"), "tp", None),
        P(("grp", "sp"), "tp", None),
        P("tp"),
        P("tp"),
        P(),
        P("tp", None),
        P("tp", None),
        P(),
        P("sp", "tp"),
        P("tp", "sp"),
    )
    return jax.shard_map(
        shards, mesh=mesh, in_specs=placed, out_specs=P(("grp", "sp", "tp"), None), check_vma=False
    )
```

```python
import functools
import math

import jax
import jax.numpy as jnp
from jax import lax
from jax.experimental import pallas as pl
from jax.experimental.pallas import tpu as pltpu
from jax.sharding import PartitionSpec as P


NORM_EPS = 1e-06
OUT_SCALE = 0.8
LOG2E = math.log2(math.e)
LAST_DIMS = (((1,), (1,)), ((), ()))
VMEM_LIMIT = 58 * 2**20
EARLY = 8


def split_up(array, dim, peers):
    before, after = (array.shape[:dim], array.shape[dim + 1 :])
    return jnp.moveaxis(array.reshape(*before, peers, -1, *after), dim, 0)


def sent_and_summed(array, axis, dim):
    peers = lax.axis_size(axis)
    parts = lax.all_to_all(split_up(array, dim, peers), axis, 0, 0, tiled=True)
    return jnp.sum(parts.astype(jnp.float32), axis=0)


def after(array, *others):
    return lax.optimization_barrier((array, *others))[0]


def copy_for_each(array, axis):
    copies = jnp.broadcast_to(array, (lax.axis_size(axis), *array.shape))
    return lax.all_to_all(copies, axis, split_axis=0, concat_axis=0, tiled=True)


def ring(block):
    peers = lax.axis_size("sp")
    chips = peers // 2
    onward = [(i, (i + 2) % peers) for i in range(peers)]
    backward = [(i, (i - 2) % peers) for i in range(peers)]
    ahead, behind = block, block
    blocks, places = [block], [0]
    for step in range(1, chips // 2 + 1):
        ahead = lax.ppermute(ahead, "sp", onward)
        blocks.append(ahead)
        places.append(-step % chips)
        if step < chips - chips // 2:
            behind = lax.ppermute(behind, "sp", backward)
            blocks.append(behind)
            places.append(step)
    return stacked(blocks), places


def stack_kernel(*refs):
    for i, block in enumerate(refs[:-1]):
        refs[-1][i] = block[...]


def stacked(blocks):
    vmem = pl.BlockSpec(memory_space=pltpu.VMEM)
    return pl.pallas_call(
        stack_kernel,
        in_specs=[vmem] * len(blocks),
        out_specs=vmem,
        out_shape=jax.ShapeDtypeStruct((len(blocks), *blocks[0].shape), blocks[0].dtype),
        compiler_params=pltpu.CompilerParams(vmem_limit_bytes=12 * 2**20),
        name="stack",
    )(*blocks)


def attend_kernel(
    qn_ref,
    qw_ref,
    kv_ref,
    lam_ref,
    gain_ref,
    rows_n_ref,
    rows_w_ref,
    out_ref,
    q_s,
    m_s,
    acc_s,
    v_s,
    att_s,
    *,
    dn,
    dw,
    dv,
    steps,
    parts,
):
    step, part = pl.program_id(0), pl.program_id(1)
    rows = qn_ref.shape[0]
    some = pl.ds(pl.multiple_of(part * (rows // parts), rows // parts), rows // parts)

    @pl.when((step == 0) & (part == 0))
    def _():
        m_s[...] = jnp.full_like(m_s, -jnp.inf)
        acc_s[...] = jnp.zeros_like(acc_s)
        v_s[...] = jnp.ones_like(v_s)
        lane = lax.broadcasted_iota(jnp.int32, (rows, 2 * dn), 1)
        for h in range(2):
            q = qn_ref[:, h * 2 * dn : (h + 1) * 2 * dn]
            for c in range(2):
                keep = (lane < dn) if c == 0 else (lane >= dn)
                q_s[h * 2 + c] = jnp.where(keep, q, jnp.zeros_like(q))
                q_s[4 + h * 2 + c] = qw_ref[:, (h * 2 + c) * dw : (h * 2 + c + 1) * dw]

    at_vn = 2 * dn
    at_kw = at_vn + dv
    at_vw = at_kw + 2 * dw

    @pl.when(part == 0)
    def _():
        v_s[0, :, :dv] = kv_ref[:, at_vn : at_vn + dv]
        v_s[1, :, :dv] = kv_ref[:, at_vw : at_vw + dv]

    for u in range(8):
        wide, c = u >= 4, u % 2
        at = at_kw + c * dw if wide else 0
        width = dw if wide else 2 * dn
        scale = (dw if wide else dn) ** -0.5 * LOG2E
        s = lax.dot_general(
            q_s[u, some], kv_ref[:, at : at + width], LAST_DIMS, preferred_element_type=jnp.float32
        )
        m_old = m_s[u, some]
        m_new = jnp.maximum(m_old, jnp.max(s, axis=1, keepdims=True))
        powers = jnp.exp2((s - m_new) * scale).astype(jnp.bfloat16)
        rescale = jnp.exp2((m_old - m_new) * scale)
        m_s[u, some] = m_new
        acc_s[u, some] = acc_s[u, some] * rescale + jnp.dot(
            powers, v_s[int(wide)], preferred_element_type=jnp.float32
        )

    @pl.when((step == steps - 1) & (part == parts - 1))
    def _():
        for h in range(4):
            first, second = acc_s[2 * h], acc_s[2 * h + 1]
            o = first[:, :dv] / first[:, dv:] - lam_ref[h] * (second[:, :dv] / second[:, dv:])
            square = jnp.mean(o * o, axis=-1, keepdims=True)
            o = o * lax.rsqrt(square + NORM_EPS) * gain_ref[...] * OUT_SCALE
            att_s[:, h * dv : (h + 1) * dv] = o.astype(att_s.dtype)
        cut = rows_n_ref.shape[0]
        total = jnp.dot(att_s[:, :cut], rows_n_ref[...], preferred_element_type=jnp.float32)
        total += jnp.dot(att_s[:, cut:], rows_w_ref[...], preferred_element_type=jnp.float32)
        out_ref[...] = total.astype(out_ref.dtype)


def attention(qn, qw, kv, lam, gain, rows_n, rows_w):
    rows = qn.shape[0]
    keys, width = kv.shape
    dv = gain.shape[1]
    dn, dw = qn.shape[1] // 4, qw.shape[1] // 4
    block = math.gcd(keys, 2048)
    steps = keys // block
    return pl.pallas_call(
        functools.partial(attend_kernel, dn=dn, dw=dw, dv=dv, steps=steps, parts=1),
        grid=(steps, 1),
        in_specs=[
            pl.BlockSpec(qn.shape, lambda i, j: (0, 0)),
            pl.BlockSpec(qw.shape, lambda i, j: (0, 0)),
            pl.BlockSpec((block, width), lambda i, j: (i, 0)),
            pl.BlockSpec(memory_space=pltpu.SMEM),
            pl.BlockSpec(gain.shape, lambda i, j: (0, 0)),
            pl.BlockSpec(rows_n.shape, lambda i, j: (0, 0)),
            pl.BlockSpec(rows_w.shape, lambda i, j: (0, 0)),
        ],
        out_specs=pl.BlockSpec((rows, rows_n.shape[1]), lambda i, j: (0, 0)),
        out_shape=jax.ShapeDtypeStruct((rows, rows_n.shape[1]), jnp.bfloat16),
        scratch_shapes=[
            pltpu.VMEM((8, rows, 128), jnp.bfloat16),
            pltpu.VMEM((8, rows, 1), jnp.float32),
            pltpu.VMEM((8, rows, 2 * dv), jnp.float32),
            pltpu.VMEM((2, block, 2 * dv), jnp.bfloat16),
            pltpu.VMEM((rows, 4 * dv), jnp.bfloat16),
        ],
        compiler_params=pltpu.CompilerParams(
            dimension_semantics=("arbitrary", "arbitrary"), vmem_limit_bytes=VMEM_LIMIT
        ),
        cost_estimate=pl.CostEstimate(
            flops=16 * rows * keys * 256, bytes_accessed=keys * width * 2, transcendentals=8 * rows * keys
        ),
        name="attend",
    )(qn, qw, kv, lam, gain, rows_n, rows_w)


def early_mixer_kernel(chip_ref, x_ref, *refs, places):
    arrays, (out_ref, w_s, x_s, out_s, sem) = refs[:-5], refs[-5:]
    chips = len(places)
    each = x_ref.shape[1] // chips
    copies = [pltpu.make_async_copy(w, w_s.at[i], sem.at[i]) for i, w in enumerate(arrays)]
    for copy in copies:
        copy.start()

    def columns(at):
        chip = lax.rem(chip_ref[0] + at, chips)
        return pl.ds(pl.multiple_of(chip * each, each), each)

    for i, at in enumerate(places):
        x_s[:, i * each : (i + 1) * each] = x_ref[:, columns(at)]
    for k, copy in enumerate(copies):
        copy.wait()
        up = w_s[k, :, :, 0].reshape(x_ref.shape[1], w_s.shape[5])
        down = w_s[k, :, :, 1].reshape(x_ref.shape[1], w_s.shape[5])
        lifted = jnp.maximum(jnp.dot(x_s[...], up, preferred_element_type=jnp.float32), 0.0)
        part = lax.dot_general(
            (lifted * lifted).astype(jnp.bfloat16),
            down,
            LAST_DIMS,
            preferred_element_type=jnp.float32,
        )
        out_s[...] = part if k == 0 else out_s[...] + part
    for i, at in enumerate(places):
        out_ref[:, columns(at)] = out_s[:, i * each : (i + 1) * each]


def early_mixer(x, weights, places):
    rows, d = x.shape
    hidden = sum(w.shape[4] for w in weights)
    chip = (lax.axis_index("sp") // 2).astype(jnp.int32).reshape(1)
    vmem = pl.BlockSpec(memory_space=pltpu.VMEM)
    return pl.pallas_call(
        functools.partial(early_mixer_kernel, places=places),
        in_specs=[
            pl.BlockSpec(memory_space=pltpu.SMEM),
            vmem,
            *(pl.BlockSpec(memory_space=pl.ANY) for _ in weights),
        ],
        out_specs=vmem,
        out_shape=jax.ShapeDtypeStruct((rows, d), jnp.float32),
        scratch_shapes=[
            pltpu.VMEM((len(weights), *weights[0].shape), weights[0].dtype),
            pltpu.VMEM((rows, d), jnp.bfloat16),
            pltpu.VMEM((rows, d), jnp.float32),
            pltpu.SemaphoreType.DMA((len(weights),)),
        ],
        compiler_params=pltpu.CompilerParams(vmem_limit_bytes=50 * 2**20),
        cost_estimate=pl.CostEstimate(
            flops=4 * rows * d * hidden, bytes_accessed=4 * d * hidden, transcendentals=0
        ),
        name="early_mixer",
    )(chip, x, *weights)


def mixer_kernel(x_ref, w_ref, early_ref, out_ref, lifted, activated, *, half):
    step = pl.program_id(0)
    depth = w_ref.shape[0] * w_ref.shape[2]
    w = w_ref[...].reshape(depth, w_ref.shape[3])

    @pl.when(step < half)
    def _():
        at = pl.multiple_of(step * depth, depth)
        part = jnp.dot(x_ref[:, pl.ds(at, depth)], w, preferred_element_type=jnp.float32)

        @pl.when(step == 0)
        def _():
            lifted[...] = part

        @pl.when(step > 0)
        def _():
            lifted[...] += part

    @pl.when(step == half - 1)
    def _():
        up = jnp.maximum(lifted[...], 0.0)
        activated[...] = (up * up).astype(jnp.bfloat16)

    @pl.when(step >= half)
    def _():
        part = lax.dot_general(activated[...], w, LAST_DIMS, preferred_element_type=jnp.float32)
        out_ref[...] = (early_ref[...] + part).astype(jnp.bfloat16)


def mixer(x, w, early):
    rows, d = x.shape
    shards, _, each, hidden = w.shape
    group = math.gcd(shards, 32)
    half = shards // group
    depth = group * each
    return pl.pallas_call(
        functools.partial(mixer_kernel, half=half),
        grid=(2 * half,),
        in_specs=[
            pl.BlockSpec((rows, d), lambda i: (0, 0)),
            pl.BlockSpec((group, 1, each, hidden), lambda i: (i % half, i // half, 0, 0)),
            pl.BlockSpec((rows, depth), lambda i: (0, jnp.maximum(i - half, 0))),
        ],
        out_specs=pl.BlockSpec((rows, depth), lambda i: (0, jnp.maximum(i - half, 0))),
        out_shape=jax.ShapeDtypeStruct((rows, d), jnp.bfloat16),
        scratch_shapes=[
            pltpu.VMEM((rows, hidden), jnp.float32),
            pltpu.VMEM((rows, hidden), jnp.bfloat16),
        ],
        compiler_params=pltpu.CompilerParams(
            dimension_semantics=("arbitrary",), vmem_limit_bytes=50 * 2**20
        ),
        cost_estimate=pl.CostEstimate(
            flops=4 * rows * d * hidden, bytes_accessed=4 * d * hidden, transcendentals=0
        ),
        name="mixer",
    )(x, w, early)


def shards(
    resid_in,
    query_narrow,
    key_narrow,
    value_narrow,
    query_wide,
    key_wide,
    value_wide,
    lambda_narrow,
    lambda_wide,
    head_gain,
    out_narrow,
    out_wide,
    norm_gain,
    up_weight,
    down_weight,
):
    rows = query_narrow.shape[0]
    sp, grp = lax.axis_size("sp"), lax.axis_size("grp")
    core, side = lax.axis_index("sp") % 2, lax.axis_index("grp") % 2
    other_core = [(i, i ^ 1) for i in range(sp)]
    other_group = [(i, i ^ 1) for i in range(grp)]
    own = jnp.concatenate(
        [a.reshape(rows, -1) for a in (key_narrow, value_narrow, key_wide, value_wide)], axis=1
    )
    kv = lax.all_gather(own, "sp", axis=0, tiled=True)
    own_weights = jnp.stack([up_weight, down_weight.T])
    hidden = up_weight.shape[1]
    share = hidden * EARLY // 16
    each = share // 4
    late_weights = lax.all_gather(own_weights[:, :, share:], "sp", axis=0, tiled=False)
    mine = lax.dynamic_slice_in_dim(own_weights, (2 * side + core) * each, each, 2)
    theirs = lax.dynamic_slice_in_dim(own_weights, (2 * side + 1 - core) * each, each, 2)
    theirs = lax.ppermute(theirs, "sp", other_core)
    chip = jnp.where(core == 0, jnp.stack([mine, theirs]), jnp.stack([theirs, mine]))
    stack, places = ring(chip)
    swapped = lax.ppermute(stack, "grp", other_group)
    first = lax.ppermute(stack, "sp", other_core)
    second = lax.ppermute(swapped, "sp", other_core)
    early_weights = (stack, first, swapped, second)
    kv = after(kv, stack)
    projected = attention(
        query_narrow.reshape(rows, -1),
        query_wide.reshape(rows, -1),
        kv,
        jnp.concatenate([lambda_narrow, lambda_wide]),
        head_gain.reshape(1, -1),
        out_narrow,
        out_wide,
    )
    projected = sent_and_summed(projected, "tp", 0)
    middle = (resid_in.astype(jnp.float32) + projected).astype(jnp.bfloat16)
    middle_f32 = middle.astype(jnp.float32)
    normed = middle_f32 * lax.rsqrt(
        jnp.mean(middle_f32 * middle_f32, axis=-1, keepdims=True) + NORM_EPS
    )
    normed = (normed * norm_gain.astype(jnp.float32)).astype(jnp.bfloat16)
    normed = copy_for_each(normed, "tp").reshape(-1, normed.shape[1])
    early = early_mixer(normed, early_weights, places)
    mixer_out = sent_and_summed(mixer(normed, late_weights, early), "tp", 0)
    return (middle_f32 + mixer_out).astype(jnp.bfloat16)


def solution(mesh):
    placed = (
        P(("grp", "sp", "tp"), None),
        P(("grp", "sp"), "tp", None),
        P(("grp", "sp"), "tp", None),
        P(("grp", "sp"), "tp", None),
        P(("grp", "sp"), "tp", None),
        P(("grp", "sp"), "tp", None),
        P(("grp", "sp"), "tp", None),
        P("tp"),
        P("tp"),
        P(),
        P("tp", None),
        P("tp", None),
        P(),
        P("sp", "tp"),
        P("tp", "sp"),
    )
    return jax.shard_map(
        shards, mesh=mesh, in_specs=placed, out_specs=P(("grp", "sp", "tp"), None), check_vma=False
    )
```
